32 devices in a mesh: sp: 8 (over z, y), tp: 4 (over x, core).
Axes of the slice: x: 2, y: 2, z: 4, core: 2. Of those that a mesh axis runs over, the one named last changes fastest.
Arguments:
- source: bfloat16 [4096, 2048], P(('sp', 'tp')), may hold values from -6 to 6
- target: bfloat16 [1024, 2048], P(('sp', 'tp')), may hold values from -6 to 6
- source_gain: bfloat16 [2, 2048], replicated, may hold values from 0.099609375 to 1.8984375
- target_gain: bfloat16 [2, 2048], replicated, may hold values from 0.099609375 to 1.8984375
- query_weight: bfloat16 [2, 2048, 1024], P(None, None, 'tp'), may hold values from -0.5 to 0.5
- key_weight: bfloat16 [2, 2048, 1024], P(None, None, 'tp'), may hold values from -0.5 to 0.5
- value_weight: bfloat16 [2, 2048, 1024], P(None, None, 'tp'), may hold values from -0.125 to 0.125
- head_gain: bfloat16 [2, 1024], P(None, 'tp'), may hold values from 0.099609375 to 1.8984375
- out_weight: bfloat16 [2, 1024, 2048], P(None, 'tp'), may hold values from -0.1875 to 0.1875
- mlp_gain: bfloat16 [2048], replicated, may hold values from 0.099609375 to 1.8984375
- gate_weight: bfloat16 [2048, 5632], P(None, 'tp'), may hold values from -0.125 to 0.125
- up_weight: bfloat16 [2048, 5632], P(None, 'tp'), may hold values from -0.125 to 0.125
- down_weight: bfloat16 [5632, 2048], P('tp'), may hold values from -0.078125 to 0.078125
Outputs:
- mixed: bfloat16 [1024, 2048], P(('sp', 'tp'))
The draws below stay inside these ranges and needn't reach their ends.
All inputs are finite; a program needn't handle non-finite values.
Results may differ from the reference program's by a relative error of at most 0.014.
Values may be sent and summed in bfloat16 or wider, within the bound.
A program may use at most 128 MiB of HBM per device.

```python
import jax
import jax.numpy as jnp
from jax import lax

D = 2048
HEADS = 8
HEAD_DIM = 128
FF = 5632
LAYERS = 2
SRC_DEV = 512
QW = 1024
TARGET = 1024
SOURCE = 4096
N_SP = 8


def source_rows(key):
    rows = jax.random.normal(jax.random.fold_in(key, 31), (SOURCE, D), jnp.float32)
    return jnp.clip(rows, -6.0, 6.0)


def draw_source(key, part):
    return source_rows(key).astype(jnp.bfloat16)


def draw_target(key, part):
    rows = jnp.clip(jax.random.normal(jax.random.fold_in(key, 33), (TARGET, D), jnp.float32), -6.0, 6.0)
    return rows.astype(jnp.bfloat16)


def own_noise(key, salt):
    return jax.random.normal(jax.random.fold_in(key, salt), (LAYERS, D, QW), jnp.float32) * D ** (-0.5)


def draw_query_weight(key, part):
    weight = jnp.clip(own_noise(key, 42), -0.5, 0.5)
    return weight.astype(jnp.bfloat16)


def draw_key_weight(key, part):
    weight = jnp.clip(own_noise(key, 43), -0.5, 0.5)
    return weight.astype(jnp.bfloat16)


def level_of(rng, shape, shards, least, high):
    def one(axis_at, blocks):
        draws = jax.random.uniform(jax.random.fold_in(jax.random.fold_in(rng, 6), axis_at), (blocks,), jnp.float32, least / len(shards), high / len(shards))
        return jnp.repeat(jnp.exp(draws), shape[axis_at] // blocks).reshape((-1,) + (1,) * (len(shape) - axis_at - 1))

    loudness = one(*shards[0])
    for cut in shards[1:]:
        loudness = loudness * one(*cut)
    return loudness


def bell_draw(own_key, shape, width, limit, shards=(), dtype=jnp.bfloat16):
    result = jax.random.normal(own_key, shape, jnp.float32) * width
    if len(shards) > 0:
        result = level_of(own_key, shape, shards, -0.22, 0.18) * result
    return jnp.clip(result, min=-limit, max=limit).astype(dtype)


def setup_inputs(seed: int = 0) -> dict:
    splits = jax.random.split(jax.random.key(seed), 14)
    return {
        "source": draw_source(jax.random.fold_in(splits[13], 71), 0),
        "target": draw_target(jax.random.fold_in(splits[13], 71), 0),
        "source_gain": jnp.clip(1.0 + 0.18 * jax.random.normal(splits[2], (LAYERS, D), jnp.float32), 0.099609375, 1.8984375).astype(jnp.bfloat16),
        "target_gain": jnp.clip(1.0 + 0.18 * jax.random.normal(splits[3], (LAYERS, D), jnp.float32), 0.099609375, 1.8984375).astype(jnp.bfloat16),
        "query_weight": draw_query_weight(jax.random.fold_in(splits[13], 71), 0),
        "key_weight": draw_key_weight(jax.random.fold_in(splits[13], 71), 0),
        "value_weight": bell_draw(splits[6], (LAYERS, D, QW), D ** -0.5, 0.125, ((2, 4),)),
        "head_gain": jnp.clip(1.0 + 0.18 * jax.random.normal(splits[7], (LAYERS, QW), jnp.float32), 0.099609375, 1.8984375).astype(jnp.bfloat16),
        "out_weight": bell_draw(splits[8], (LAYERS, QW, D), QW ** -0.5, 0.1875, ((1, 4),)),
        "mlp_gain": jnp.clip(1.0 + 0.18 * jax.random.normal(splits[9], (D,), jnp.float32), 0.099609375, 1.8984375).astype(jnp.bfloat16),
        "gate_weight": bell_draw(splits[10], (D, FF), D ** -0.5, 0.125, ((1, 4),)),
        "up_weight": bell_draw(splits[11], (D, FF), D ** -0.5, 0.125, ((1, 4),)),
        "down_weight": bell_draw(splits[12], (FF, D), FF ** -0.5, 0.078125, ((0, 4),)),
    }


EPSILON = 1e-06

def row_scale(rows):
    return lax.rsqrt(lax.optimization_barrier(jnp.mean(rows * rows, axis=-1, keepdims=True)) + EPSILON)

def block_stats(queries, key_blocks, value_blocks):
    scores = jnp.einsum('the,bshe->bhts', queries.astype(jnp.float32), key_blocks.astype(jnp.float32), precision=lax.Precision.HIGHEST) * HEAD_DIM ** (-0.5)
    block_max = lax.optimization_barrier(jnp.max(scores, axis=-1))
    weights = jnp.exp(scores - block_max[..., None])
    block_total = lax.optimization_barrier(jnp.sum(weights, axis=-1))
    weights_low = lax.optimization_barrier(weights.astype(jnp.bfloat16))
    block_out = jnp.einsum('bhts,bshe->bthe', weights_low.astype(jnp.float32), value_blocks.astype(jnp.float32), precision=lax.Precision.HIGHEST).astype(jnp.bfloat16)
    return (jnp.swapaxes(block_max, 1, 2), jnp.swapaxes(block_total, 1, 2), block_out)

def merge_blocks(carry, stats):
    run_max, run_total, run_out = carry
    block_max, block_total, block_out = stats
    new_max = jnp.maximum(run_max, lax.optimization_barrier(jnp.max(block_max, axis=0)))
    keep = jnp.exp(run_max - new_max)
    factor = jnp.exp(block_max - new_max[None])
    total = run_total * keep + lax.optimization_barrier(jnp.sum(factor * block_total, axis=0))
    widened = lax.optimization_barrier(block_out).astype(jnp.float32)
    out = run_out * keep[..., None] + lax.optimization_barrier(jnp.sum(factor[..., None] * widened, axis=0))
    return (new_max, total, out)

def reference(source, target, source_gain, target_gain, query_weight, key_weight, value_weight, head_gain, out_weight, mlp_gain, gate_weight, up_weight, down_weight):
    src_wide = source.astype(jnp.float32)
    src_scale = row_scale(src_wide)
    state = target
    for layer in range(LAYERS):
        src_normed = (src_wide * src_scale * source_gain[layer].astype(jnp.float32)).astype(jnp.bfloat16)
        keys = jnp.dot(src_normed, key_weight[layer], preferred_element_type=jnp.float32).astype(jnp.bfloat16)
        values = jnp.dot(src_normed, value_weight[layer], preferred_element_type=jnp.float32).astype(jnp.bfloat16)
        keys = keys.reshape(N_SP, SRC_DEV, HEADS, HEAD_DIM)
        values = values.reshape(N_SP, SRC_DEV, HEADS, HEAD_DIM)
        state_wide = state.astype(jnp.float32)
        tgt_normed = (state_wide * row_scale(state_wide) * target_gain[layer].astype(jnp.float32)).astype(jnp.bfloat16)
        queries = jnp.dot(tgt_normed, query_weight[layer], preferred_element_type=jnp.float32).astype(jnp.bfloat16)
        queries = queries.reshape(TARGET, HEADS, HEAD_DIM)

        def advance(carry, pair):
            return (merge_blocks(carry, block_stats(queries, pair[0][None], pair[1][None])), None)
        start = (jnp.full((TARGET, HEADS), -jnp.inf, jnp.float32), jnp.zeros((TARGET, HEADS), jnp.float32), jnp.zeros((TARGET, HEADS, HEAD_DIM), jnp.float32))
        (run_max, run_total, run_out), _ = lax.scan(advance, start, (keys, values))
        attended = run_out / run_total[..., None]
        head_out = attended * row_scale(attended) * head_gain[layer].astype(jnp.float32).reshape(HEADS, HEAD_DIM)
        head_out = head_out.astype(jnp.bfloat16).reshape(TARGET, QW)
        projected = jnp.dot(head_out, out_weight[layer], preferred_element_type=jnp.float32)
        state = (state.astype(jnp.float32) + projected).astype(jnp.bfloat16)
    state_wide = state.astype(jnp.float32)
    mlp_in = (state_wide * row_scale(state_wide) * mlp_gain.astype(jnp.float32)).astype(jnp.bfloat16)
    gate = jnp.dot(mlp_in, gate_weight, preferred_element_type=jnp.float32)
    upward = jnp.dot(mlp_in, up_weight, preferred_element_type=jnp.float32)
    hidden = (jax.nn.silu(gate) * upward).astype(jnp.bfloat16)
    down = jnp.dot(hidden, down_weight, preferred_element_type=jnp.float32)
    return (state_wide + 0.5 * down).astype(jnp.bfloat16)
```

```python
import functools

import jax
import jax.numpy as jnp
from jax import lax
from jax.experimental import pallas as pl
from jax.experimental.pallas import tpu as pltpu
from jax.sharding import PartitionSpec as P

HEAD_DIM = 128
EPSILON = 1e-06
LOG2E = 1.4426950408889634
CHUNKS = 4
TILE = 256
BF = jnp.bfloat16
F32 = jnp.float32


def rms(rows):
    return rows * lax.rsqrt(jnp.mean(rows * rows, axis=-1, keepdims=True) + EPSILON)


def dot(a, b):
    return jnp.dot(a, b, preferred_element_type=F32)


def dot_nt(a, b):
    return lax.dot_general(a, b, (((1,), (1,)), ((), ())), preferred_element_type=F32)


def merge(parts):
    top = functools.reduce(jnp.maximum, [m for _, m, _ in parts])
    out, total = 0.0, 0.0
    for o, m, t in parts:
        factor = jnp.exp2(m - top)
        out = out + factor * o.astype(F32)
        total = total + factor * t
    return out, top, total


def kernel(
    n_sp, n_tp,
    target, source_gain, target_gain, head_gain, mlp_gain,
    source, *rest,
):
    weights_hbm = rest[:7]
    out_ref = rest[7]
    (src, xs, qw, kw, vw, ow, gw, uw, dw, nrm, kbuf, vbuf, qbuf, head,
     o_own, s_own, o_snd, s_snd, o_p1, s_p1, o_mrg, s_mrg, o_r2, s_r2,
     r_own, r_snd, r_p1, r_mrg, r_r2, hid, load_sem, send_sem, recv_sem) = rest[8:]
    layers = qw.shape[0]
    heads = qw.shape[2] // HEAD_DIM
    width = xs.shape[3]
    rows = xs.shape[2]
    group = rows * n_tp
    src_rows = src.shape[1]
    cols = width // CHUNKS
    n_x, n_p = n_tp // 2, n_sp // 2
    sp, tp = lax.axis_index("sp"), lax.axis_index("tp")
    where = {"sp": (sp // 2, sp % 2, n_p), "tp": (tp // 2, tp % 2, n_x)}

    def peer(axis, shift):
        pair, side, count = where[axis]
        return {axis: ((pair + shift + count) % count) * 2 + side}

    def partner(axis):
        pair, side, _ = where[axis]
        return {axis: pair * 2 + 1 - side}

    copies = []

    def remote(src_ref, dst_ref, device):
        number = len(copies)
        copy = pltpu.make_async_remote_copy(
            src_ref=src_ref, dst_ref=dst_ref,
            send_sem=send_sem.at[number], recv_sem=recv_sem.at[number],
            device_id=device, device_id_type=pl.DeviceIdType.MESH,
        )
        copy.start()
        copies.append(copy)
        return copy

    loads = {}

    def load(name, src_ref, dst_ref):
        copy = pltpu.make_async_copy(src_ref, dst_ref, load_sem.at[len(loads)])
        copy.start()
        loads[name] = copy

    qh, kh, vh, oh, gh, uh, dh = weights_hbm
    load("src", source, src.at[0])
    for l in range(layers):
        load(("q", l), qh.at[l], qw.at[l])
        load(("k", l), kh.at[l], kw.at[l])
        load(("v", l), vh.at[l], vw.at[l])
        load(("o", l), oh.at[l], ow.at[l])
    load("g", gh, gw)
    load("u", uh, uw)
    load("d", dh, dw)

    barrier = pltpu.get_barrier_semaphore()
    others = [peer("tp", k) for k in range(1, n_x)] + [peer("sp", k) for k in range(1, n_p)]
    others += [partner("tp"), partner("sp")]
    for device in others:
        pl.semaphore_signal(barrier, inc=1, device_id=device, device_id_type=pl.DeviceIdType.MESH)
    pl.semaphore_wait(barrier, len(others))

    class Gather:
        def __init__(self, own, buf, axis):
            self.buf, self.axis = buf, axis
            self.count = where[axis][2]
            self.far = {k: remote(own, buf.at[2 * k], peer(axis, k)) for k in range(1, self.count)}
            self.near = {0: remote(own, buf.at[1], partner(axis))}

        def forward(self, k):
            self.far[k].wait_recv()
            self.near[k] = remote(
                self.buf.at[2 * k], self.buf.at[2 * k + 1], partner(self.axis)
            )

        def forward_all(self):
            for k in range(1, self.count):
                self.forward(k)

        def wait_near(self, k):
            self.near[k].wait_recv()

        def wait_all(self):
            for k in range(self.count):
                self.wait_near(k)

    def project_source(layer, slot):
        normed = rms(src[slot].astype(F32)) * source_gain[pl.ds(layer, 1), :].astype(F32)
        normed = normed.astype(BF)
        span = pl.ds(slot * src_rows, src_rows)
        kbuf[span, :] = dot(normed, kw[layer]).astype(BF)
        vbuf[:, span] = dot(normed, vw[layer]).T.astype(BF)

    def attend(layer, slot):
        parts = []
        for h in range(heads):
            span = pl.ds(h * HEAD_DIM, HEAD_DIM)
            scores = dot_nt(kbuf[:, span], qbuf[layer, slot, :, span]) * (
                HEAD_DIM ** (-0.5) * LOG2E
            )
            top = jnp.max(scores, axis=0, keepdims=True)
            weights = jnp.exp2(scores - top)
            total = jnp.sum(weights, axis=0, keepdims=True)
            parts.append((dot(vbuf[span, :], weights.astype(BF)), top, total))
        return parts

    def put(parts, out, stats):
        for h, (o, m, t) in enumerate(parts):
            out[pl.ds(h * HEAD_DIM, HEAD_DIM), :] = o.astype(out.dtype)
            stats[pl.ds(h, 1), :] = m
            stats[pl.ds(heads + h, 1), :] = t

    def get(out, stats, h):
        return (
            out[pl.ds(h * HEAD_DIM, HEAD_DIM), :],
            stats[pl.ds(h, 1), :],
            stats[pl.ds(heads + h, 1), :],
        )

    def reduce_scatter(phase, part):
        first, second = {}, {}

        def pass_on(j):
            for k in range(1, n_x):
                first[j, k].wait_recv()
                r_mrg[phase, j, k] = (
                    r_own[k, :, pl.ds(j * cols, cols)] + r_p1[phase, j, k].astype(F32)
                ).astype(BF)
                second[j, k] = remote(
                    r_mrg.at[phase, j, k], r_r2.at[phase, j, k], peer("tp", -k)
                )

        for j in range(CHUNKS):
            piece = part(j)
            for k in list(range(1, n_x)) + [0]:
                mine, other = 2 * k * rows, (2 * k + 1) * rows
                r_own[k, :, pl.ds(j * cols, cols)] = piece[mine : mine + rows]
                r_snd[phase, j, k] = piece[other : other + rows].astype(BF)
                first[j, k] = remote(r_snd.at[phase, j, k], r_p1.at[phase, j, k], partner("tp"))
            if j:
                pass_on(j - 1)
        pass_on(CHUNKS - 1)
        for j in range(CHUNKS):
            first[j, 0].wait_recv()
            total = r_own[0, :, pl.ds(j * cols, cols)] + r_p1[phase, j, 0].astype(F32)
            for k in range(1, n_x):
                second[j, k].wait_recv()
                total = total + r_r2[phase, j, k].astype(F32)
            yield pl.ds(j * cols, cols), total

    def norm_rows(phase, gain):
        for s in range(n_tp):
            nrm[pl.ds(s * rows, rows), :] = (rms(xs[phase, s].astype(F32)) * gain).astype(BF)

    rows_in = Gather(target, xs.at[0], "tp")
    xs[0, 0] = target[...]
    loads["src"].wait()
    source_in = Gather(src.at[0], src, "tp")

    for l in range(layers):
        rows_in.forward_all()
        rows_in.wait_all()
        norm_rows(l, target_gain[pl.ds(l, 1), :].astype(F32))
        loads["q", l].wait()
        qbuf[l, 0] = dot(nrm[...], qw[l]).astype(BF)
        queries = Gather(qbuf.at[l, 0], qbuf.at[l], "sp")
        if l == 0:
            loads["k", l].wait()
            loads["v", l].wait()
            project_source(l, 0)
            source_in.wait_near(0)
            project_source(l, 1)
        queries.forward_all()
        if l == 0:
            source_in.forward_all()
            for k in range(1, n_x):
                project_source(l, 2 * k)
                source_in.wait_near(k)
                project_source(l, 2 * k + 1)
        near_o, near_s, far_o, far_s = {}, {}, {}, {}

        def pass_on(k, l=l, near_o=near_o, near_s=near_s, far_o=far_o, far_s=far_s):
            near_o[k].wait_recv()
            near_s[k].wait_recv()
            merged = [
                merge([get(o_own.at[k], s_own.at[k], h), get(o_p1.at[l, k], s_p1.at[l, k], h)])
                for h in range(heads)
            ]
            put(merged, o_mrg.at[l, k], s_mrg.at[l, k])
            far_s[k] = remote(s_mrg.at[l, k], s_r2.at[l, k], peer("sp", -k))
            far_o[k] = remote(o_mrg.at[l, k], o_r2.at[l, k], peer("sp", -k))

        order = list(range(1, n_p)) + [0]
        for step, k in enumerate(order):
            put(attend(l, 2 * k), o_own.at[k], s_own.at[k])
            queries.wait_near(k)
            put(attend(l, 2 * k + 1), o_snd.at[l, k], s_snd.at[l, k])
            near_s[k] = remote(s_snd.at[l, k], s_p1.at[l, k], partner("sp"))
            near_o[k] = remote(o_snd.at[l, k], o_p1.at[l, k], partner("sp"))
            if step:
                pass_on(order[step - 1])
        if l + 1 < layers:
            loads["k", l + 1].wait()
            loads["v", l + 1].wait()
            for slot in range(n_tp):
                project_source(l + 1, slot)
        near_o[0].wait_recv()
        near_s[0].wait_recv()
        for k in range(1, n_p):
            far_s[k].wait_recv()
            far_o[k].wait_recv()
        for h in range(heads):
            parts = [get(o_own.at[0], s_own.at[0], h), get(o_p1.at[l, 0], s_p1.at[l, 0], h)]
            parts += [get(o_r2.at[l, k], s_r2.at[l, k], h) for k in range(1, n_p)]
            out, _, total = merge(parts)
            attended = out / total
            attended = attended * lax.rsqrt(
                jnp.mean(attended * attended, axis=0, keepdims=True) + EPSILON
            )
            span = pl.ds(h * HEAD_DIM, HEAD_DIM)
            head[:, span] = (
                attended.T * head_gain[pl.ds(l, 1), span].astype(F32)
            ).astype(BF)
        loads["o", l].wait()

        def share(j, l=l):
            return dot(head[...], ow[l, :, pl.ds(j * cols, cols)])

        for span, total in reduce_scatter(l, share):
            xs[l + 1, 0, :, span] = (xs[l, 0, :, span].astype(F32) + total).astype(BF)
        rows_in = Gather(xs.at[l + 1, 0], xs.at[l + 1], "tp")

    rows_in.forward_all()
    rows_in.wait_all()
    norm_rows(layers, mlp_gain[...].astype(F32))
    loads["g"].wait()
    loads["u"].wait()
    units = gw.shape[1]
    for begin in range(0, units, TILE):
        span = pl.ds(begin, min(TILE, units - begin))
        gate = dot(nrm[...], gw[:, span])
        upward = dot(nrm[...], uw[:, span])
        hid[:, span] = (gate / (1.0 + jnp.exp(-gate)) * upward).astype(BF)
    loads["d"].wait()

    def down(j):
        return dot(hid[...], dw[:, pl.ds(j * cols, cols)])

    for span, total in reduce_scatter(layers, down):
        out_ref[:, span] = (xs[layers, 0, :, span].astype(F32) + 0.5 * total).astype(BF)
    for copy in copies:
        copy.wait_send()


def local(
    n_sp, n_tp,
    source, target, source_gain, target_gain, query_weight, key_weight, value_weight,
    head_gain, out_weight, mlp_gain, gate_weight, up_weight, down_weight,
):
    layers, width, qwidth = query_weight.shape
    rows, src_rows, units = target.shape[0], source.shape[0], gate_weight.shape[1]
    group, n_x, n_p = rows * n_tp, n_tp // 2, n_sp // 2
    cols = width // CHUNKS
    total = (layers + 2) * (2 * n_x - 1) + layers * 3 * (2 * n_p - 1)
    total += (layers + 1) * CHUNKS * (2 * n_x - 1)
    vm = pltpu.VMEM
    wide, thin = (layers, n_p, qwidth, group), (layers, n_p, 8, group)
    summed = (layers + 1, CHUNKS, n_x, rows, cols)
    scratch = [
        vm((n_tp, src_rows, width), BF),
        vm((layers + 1, n_tp, rows, width), BF),
        vm((layers, width, qwidth), BF),
        vm((layers, width, qwidth), BF),
        vm((layers, width, qwidth), BF),
        vm((layers, qwidth, width), BF),
        vm((width, units), BF),
        vm((width, units), BF),
        vm((units, width), BF),
        vm((group, width), BF),
        vm((n_tp * src_rows, qwidth), BF),
        vm((qwidth, n_tp * src_rows), BF),
        vm((layers, n_sp, group, qwidth), BF),
        vm((group, qwidth), BF),
        vm(wide[1:], F32), vm(thin[1:], F32),
        vm(wide, BF), vm(thin, F32),
        vm(wide, BF), vm(thin, F32),
        vm(wide, BF), vm(thin, F32),
        vm(wide, BF), vm(thin, F32),
        vm((n_x, rows, width), F32),
        vm(summed, BF), vm(summed, BF), vm(summed, BF), vm(summed, BF),
        vm((group, units), BF),
        pltpu.SemaphoreType.DMA((4 * layers + 4,)),
        pltpu.SemaphoreType.DMA((total,)),
        pltpu.SemaphoreType.DMA((total,)),
    ]
    inside = pl.BlockSpec(memory_space=pltpu.VMEM)
    outside = pl.BlockSpec(memory_space=pl.ANY)
    return pl.pallas_call(
        functools.partial(kernel, n_sp, n_tp),
        out_shape=jax.ShapeDtypeStruct((rows, width), BF),
        in_specs=[inside] * 5 + [outside] * 8,
        out_specs=inside,
        scratch_shapes=scratch,
        compiler_params=pltpu.CompilerParams(
            collective_id=0, has_side_effects=True, vmem_limit_bytes=60 * 1024 * 1024
        ),
        name="decoder_step",
    )(
        target, source_gain, target_gain, head_gain, mlp_gain.reshape(1, width),
        source, query_weight, key_weight, value_weight, out_weight,
        gate_weight, up_weight, down_weight,
    )


def solution(mesh):
    in_specs = (
        P(("sp", "tp"), None),
        P(("sp", "tp"), None),
        P(),
        P(),
        P(None, None, "tp"),
        P(None, None, "tp"),
        P(None, None, "tp"),
        P(None, "tp"),
        P(None, "tp", None),
        P(),
        P(None, "tp"),
        P(None, "tp"),
        P("tp", None),
    )
    out_specs = P(("sp", "tp"), None)
    run = functools.partial(local, mesh.shape["sp"], mesh.shape["tp"])
    return jax.shard_map(run, mesh=mesh, in_specs=in_specs, out_specs=out_specs, check_vma=False)
```

```python
import functools

import jax
import jax.numpy as jnp
from jax import lax
from jax.experimental import pallas as pl
from jax.experimental.pallas import tpu as pltpu
from jax.sharding import PartitionSpec as P

HEAD_DIM = 128
EPSILON = 1e-06
LOG2E = 1.4426950408889634
CHUNKS = 4
TILE = 256
BF = jnp.bfloat16
F32 = jnp.float32


def rms(rows):
    return rows * lax.rsqrt(jnp.mean(rows * rows, axis=-1, keepdims=True) + EPSILON)


def dot(a, b):
    return jnp.dot(a, b, preferred_element_type=F32)


def dot_nt(a, b):
    return lax.dot_general(a, b, (((1,), (1,)), ((), ())), preferred_element_type=F32)


def merge(parts):
    top = functools.reduce(jnp.maximum, [m for _, m, _ in parts])
    out, total = 0.0, 0.0
    for o, m, t in parts:
        factor = jnp.exp2(m - top)
        out = out + factor * o.astype(F32)
        total = total + factor * t
    return out, top, total


def kernel(
    n_sp, n_tp,
    target, source_gain, target_gain, head_gain, mlp_gain,
    source, *rest,
):
    weights_hbm = rest[:7]
    out_ref = rest[7]
    (src, xs, qw, kw, vw, ow, gw, uw, dw, nrm, kbuf, vbuf, qbuf, head,
     o_own, s_own, o_snd, s_snd, o_p1, s_p1, o_mrg, s_mrg, o_r2, s_r2,
     r_own, r_snd, r_p1, r_mrg, r_r2, hid, load_sem, send_sem, recv_sem) = rest[8:]
    layers = qw.shape[0]
    heads = qw.shape[2] // HEAD_DIM
    width = xs.shape[3]
    rows = xs.shape[2]
    group = rows * n_tp
    src_rows = src.shape[1]
    cols = width // CHUNKS
    n_x, n_p = n_tp // 2, n_sp // 2
    sp, tp = lax.axis_index("sp"), lax.axis_index("tp")
    where = {"sp": (sp // 2, sp % 2, n_p), "tp": (tp // 2, tp % 2, n_x)}

    def peer(axis, shift):
        pair, side, count = where[axis]
        return {axis: ((pair + shift + count) % count) * 2 + side}

    def partner(axis):
        pair, side, _ = where[axis]
        return {axis: pair * 2 + 1 - side}

    copies = []

    def remote(src_ref, dst_ref, device):
        number = len(copies)
        copy = pltpu.make_async_remote_copy(
            src_ref=src_ref, dst_ref=dst_ref,
            send_sem=send_sem.at[number], recv_sem=recv_sem.at[number],
            device_id=device, device_id_type=pl.DeviceIdType.MESH,
        )
        copy.start()
        copies.append(copy)
        return copy

    loads = {}

    def load(name, src_ref, dst_ref):
        copy = pltpu.make_async_copy(src_ref, dst_ref, load_sem.at[len(loads)])
        copy.start()
        loads[name] = copy

    qh, kh, vh, oh, gh, uh, dh = weights_hbm
    load("src", source, src.at[0])
    for l in range(layers):
        load(("q", l), qh.at[l], qw.at[l])
        load(("k", l), kh.at[l], kw.at[l])
        load(("v", l), vh.at[l], vw.at[l])
        load(("o", l), oh.at[l], ow.at[l])
    load("g", gh, gw)
    load("u", uh, uw)
    load("d", dh, dw)

    barrier = pltpu.get_barrier_semaphore()
    others = [peer("tp", k) for k in range(1, n_x)] + [peer("sp", k) for k in range(1, n_p)]
    others += [partner("tp"), partner("sp")]
    for device in others:
        pl.semaphore_signal(barrier, inc=1, device_id=device, device_id_type=pl.DeviceIdType.MESH)
    pl.semaphore_wait(barrier, len(others))

    class Gather:
        def __init__(self, own, buf, axis):
            self.buf, self.axis = buf, axis
            self.count = where[axis][2]
            self.far = {k: remote(own, buf.at[2 * k], peer(axis, k)) for k in range(1, self.count)}
            self.near = {0: remote(own, buf.at[1], partner(axis))}

        def forward(self, k):
            self.far[k].wait_recv()
            self.near[k] = remote(
                self.buf.at[2 * k], self.buf.at[2 * k + 1], partner(self.axis)
            )

        def forward_all(self):
            for k in range(1, self.count):
                self.forward(k)

        def wait_near(self, k):
            self.near[k].wait_recv()

        def wait_all(self):
            for k in range(self.count):
                self.wait_near(k)

    class RowGather:
        def __init__(self, phase):
            self.phase = phase
            self.far, self.near = {}, {}

        def part(self, slot, j):
            return xs.at[self.phase, slot, :, pl.ds(j * cols, cols)]

        def send(self, j):
            for k in range(1, n_x):
                self.far[j, k] = remote(self.part(0, j), self.part(2 * k, j), peer("tp", k))
            self.near[j, 0] = remote(self.part(0, j), self.part(1, j), partner("tp"))

        def normalize(self, gain):
            def norm(slot):
                piece = rms(xs[self.phase, slot].astype(F32)) * gain
                nrm[pl.ds(slot * rows, rows), :] = piece.astype(BF)

            norm(0)
            for k in range(n_x):
                if k:
                    for j in range(CHUNKS):
                        self.far[j, k].wait_recv()
                        self.near[j, k] = remote(
                            self.part(2 * k, j), self.part(2 * k + 1, j), partner("tp")
                        )
                    norm(2 * k)
                for j in range(CHUNKS):
                    self.near[j, k].wait_recv()
                norm(2 * k + 1)

    def project_source(layer, slot):
        normed = rms(src[slot].astype(F32)) * source_gain[pl.ds(layer, 1), :].astype(F32)
        normed = normed.astype(BF)
        span = pl.ds(slot * src_rows, src_rows)
        kbuf[span, :] = dot(normed, kw[layer]).astype(BF)
        vbuf[:, span] = dot(normed, vw[layer]).T.astype(BF)

    def attend(layer, slot):
        parts = []
        for h in range(heads):
            span = pl.ds(h * HEAD_DIM, HEAD_DIM)
            scores = dot_nt(kbuf[:, span], qbuf[layer, slot, :, span]) * (
                HEAD_DIM ** (-0.5) * LOG2E
            )
            top = jnp.max(scores, axis=0, keepdims=True)
            weights = jnp.exp2(scores - top)
            total = jnp.sum(weights, axis=0, keepdims=True)
            parts.append((dot(vbuf[span, :], weights.astype(BF)), top, total))
        return parts

    def put(parts, out, stats):
        for h, (o, m, t) in enumerate(parts):
            out[pl.ds(h * HEAD_DIM, HEAD_DIM), :] = o.astype(out.dtype)
            stats[pl.ds(h, 1), :] = m
            stats[pl.ds(heads + h, 1), :] = t

    def get(out, stats, h):
        return (
            out[pl.ds(h * HEAD_DIM, HEAD_DIM), :],
            stats[pl.ds(h, 1), :],
            stats[pl.ds(heads + h, 1), :],
        )

    def reduce_scatter(phase, part):
        first, second = {}, {}

        def pass_on(j):
            for k in range(1, n_x):
                first[j, k].wait_recv()
                r_mrg[phase, j, k] = (
                    r_own[k, :, pl.ds(j * cols, cols)] + r_p1[phase, j, k].astype(F32)
                ).astype(BF)
                second[j, k] = remote(
                    r_mrg.at[phase, j, k], r_r2.at[phase, j, k], peer("tp", -k)
                )

        for j in range(CHUNKS):
            piece = part(j)
            for k in list(range(1, n_x)) + [0]:
                mine, other = 2 * k * rows, (2 * k + 1) * rows
                r_own[k, :, pl.ds(j * cols, cols)] = piece[mine : mine + rows]
                r_snd[phase, j, k] = piece[other : other + rows].astype(BF)
                first[j, k] = remote(r_snd.at[phase, j, k], r_p1.at[phase, j, k], partner("tp"))
            if j:
                pass_on(j - 1)
        pass_on(CHUNKS - 1)
        for j in range(CHUNKS):
            first[j, 0].wait_recv()
            total = r_own[0, :, pl.ds(j * cols, cols)] + r_p1[phase, j, 0].astype(F32)
            for k in range(1, n_x):
                second[j, k].wait_recv()
                total = total + r_r2[phase, j, k].astype(F32)
            yield pl.ds(j * cols, cols), total

    xs[0, 0] = target[...]
    rows_in = RowGather(0)
    for j in range(CHUNKS):
        rows_in.send(j)
    loads["src"].wait()
    source_in = Gather(src.at[0], src, "tp")

    for l in range(layers):
        rows_in.normalize(target_gain[pl.ds(l, 1), :].astype(F32))
        loads["q", l].wait()
        qbuf[l, 0] = dot(nrm[...], qw[l]).astype(BF)
        queries = Gather(qbuf.at[l, 0], qbuf.at[l], "sp")
        if l == 0:
            loads["k", l].wait()
            loads["v", l].wait()
            project_source(l, 0)
            source_in.wait_near(0)
            project_source(l, 1)
        if l == 0:
            queries.forward_all()
            source_in.forward_all()
            for k in range(1, n_x):
                project_source(l, 2 * k)
                source_in.wait_near(k)
                project_source(l, 2 * k + 1)
        near_o, near_s, far_o, far_s = {}, {}, {}, {}

        def pass_on(k, l=l, near_o=near_o, near_s=near_s, far_o=far_o, far_s=far_s):
            near_o[k].wait_recv()
            near_s[k].wait_recv()
            merged = [
                merge([get(o_own.at[k], s_own.at[k], h), get(o_p1.at[l, k], s_p1.at[l, k], h)])
                for h in range(heads)
            ]
            put(merged, o_mrg.at[l, k], s_mrg.at[l, k])
            far_s[k] = remote(s_mrg.at[l, k], s_r2.at[l, k], peer("sp", -k))
            far_o[k] = remote(o_mrg.at[l, k], o_r2.at[l, k], peer("sp", -k))

        def attend_near(k, l=l, queries=queries):
            queries.wait_near(k)
            put(attend(l, 2 * k + 1), o_snd.at[l, k], s_snd.at[l, k])

        def send_near(k, l=l, near_o=near_o, near_s=near_s):
            near_s[k] = remote(s_snd.at[l, k], s_p1.at[l, k], partner("sp"))
            near_o[k] = remote(o_snd.at[l, k], o_p1.at[l, k], partner("sp"))

        def forward(k, l=l, queries=queries):
            if l and k < n_p:
                queries.forward(k)

        put(attend(l, 0), o_own.at[0], s_own.at[0])
        forward(1)
        attend_near(0)
        forward(2)
        for k in range(1, n_p):
            put(attend(l, 2 * k), o_own.at[k], s_own.at[k])
            forward(k + 2)
            attend_near(k)
            send_near(k)
            if k > 1:
                pass_on(k - 1)
        send_near(0)
        pass_on(n_p - 1)
        if l + 1 < layers:
            loads["k", l + 1].wait()
            loads["v", l + 1].wait()
            for slot in range(n_tp):
                project_source(l + 1, slot)
        near_o[0].wait_recv()
        near_s[0].wait_recv()
        for k in range(1, n_p):
            far_s[k].wait_recv()
            far_o[k].wait_recv()
        for h in range(heads):
            parts = [get(o_own.at[0], s_own.at[0], h), get(o_p1.at[l, 0], s_p1.at[l, 0], h)]
            parts += [get(o_r2.at[l, k], s_r2.at[l, k], h) for k in range(1, n_p)]
            out, _, total = merge(parts)
            attended = out / total
            attended = attended * lax.rsqrt(
                jnp.mean(attended * attended, axis=0, keepdims=True) + EPSILON
            )
            span = pl.ds(h * HEAD_DIM, HEAD_DIM)
            head[:, span] = (
                attended.T * head_gain[pl.ds(l, 1), span].astype(F32)
            ).astype(BF)
        loads["o", l].wait()

        def share(j, l=l):
            return dot(head[...], ow[l, :, pl.ds(j * cols, cols)])

        rows_in = RowGather(l + 1)
        for j, (span, total) in enumerate(reduce_scatter(l, share)):
            xs[l + 1, 0, :, span] = (xs[l, 0, :, span].astype(F32) + total).astype(BF)
            rows_in.send(j)

    rows_in.normalize(mlp_gain[...].astype(F32).reshape(1, width))
    loads["g"].wait()
    loads["u"].wait()
    units = gw.shape[1]
    for begin in range(0, units, TILE):
        span = pl.ds(begin, min(TILE, units - begin))
        gate = dot(nrm[...], gw[:, span])
        upward = dot(nrm[...], uw[:, span])
        hid[:, span] = (gate / (1.0 + jnp.exp(-gate)) * upward).astype(BF)
    loads["d"].wait()

    def down(j):
        return dot(hid[...], dw[:, pl.ds(j * cols, cols)])

    for span, total in reduce_scatter(layers, down):
        out_ref[:, span] = (xs[layers, 0, :, span].astype(F32) + 0.5 * total).astype(BF)
    for copy in copies:
        copy.wait_send()


def local(
    n_sp, n_tp,
    source, target, source_gain, target_gain, query_weight, key_weight, value_weight,
    head_gain, out_weight, mlp_gain, gate_weight, up_weight, down_weight,
):
    layers, width, qwidth = query_weight.shape
    rows, src_rows, units = target.shape[0], source.shape[0], gate_weight.shape[1]
    group, n_x, n_p = rows * n_tp, n_tp // 2, n_sp // 2
    cols = width // CHUNKS
    total = ((layers + 1) * CHUNKS + 1) * (2 * n_x - 1) + layers * 3 * (2 * n_p - 1)
    total += (layers + 1) * CHUNKS * (2 * n_x - 1)
    vm = pltpu.VMEM
    wide, thin = (layers, n_p, qwidth, group), (layers, n_p, 8, group)
    summed = (layers + 1, CHUNKS, n_x, rows, cols)
    scratch = [
        vm((n_tp, src_rows, width), BF),
        vm((layers + 1, n_tp, rows, width), BF),
        vm((layers, width, qwidth), BF),
        vm((layers, width, qwidth), BF),
        vm((layers, width, qwidth), BF),
        vm((layers, qwidth, width), BF),
        vm((width, units), BF),
        vm((width, units), BF),
        vm((units, width), BF),
        vm((group, width), BF),
        vm((n_tp * src_rows, qwidth), BF),
        vm((qwidth, n_tp * src_rows), BF),
        vm((layers, n_sp, group, qwidth), BF),
        vm((group, qwidth), BF),
        vm(wide[1:], F32), vm(thin[1:], F32),
        vm(wide, BF), vm(thin, F32),
        vm(wide, BF), vm(thin, F32),
        vm(wide, BF), vm(thin, F32),
        vm(wide, BF), vm(thin, F32),
        vm((n_x, rows, width), F32),
        vm(summed, BF), vm(summed, BF), vm(summed, BF), vm(summed, BF),
        vm((group, units), BF),
        pltpu.SemaphoreType.DMA((4 * layers + 4,)),
        pltpu.SemaphoreType.DMA((total,)),
        pltpu.SemaphoreType.DMA((total,)),
    ]
    inside = pl.BlockSpec(memory_space=pltpu.VMEM)
    outside = pl.BlockSpec(memory_space=pl.ANY)
    return pl.pallas_call(
        functools.partial(kernel, n_sp, n_tp),
        out_shape=jax.ShapeDtypeStruct((rows, width), BF),
        in_specs=[inside] * 5 + [outside] * 8,
        out_specs=inside,
        scratch_shapes=scratch,
        compiler_params=pltpu.CompilerParams(
            collective_id=0, has_side_effects=True, vmem_limit_bytes=60 * 1024 * 1024
        ),
        name="decoder_step",
    )(
        target, source_gain, target_gain, head_gain, mlp_gain,
        source, query_weight, key_weight, value_weight, out_weight,
        gate_weight, up_weight, down_weight,
    )


def solution(mesh):
    in_specs = (
        P(("sp", "tp"), None),
        P(("sp", "tp"), None),
        P(),
        P(),
        P(None, None, "tp"),
        P(None, None, "tp"),
        P(None, None, "tp"),
        P(None, "tp"),
        P(None, "tp", None),
        P(),
        P(None, "tp"),
        P(None, "tp"),
        P("tp", None),
    )
    out_specs = P(("sp", "tp"), None)
    run = functools.partial(local, mesh.shape["sp"], mesh.shape["tp"])
    return jax.shard_map(run, mesh=mesh, in_specs=in_specs, out_specs=out_specs, check_vma=False)
```
